256 devices in a mesh: fs: 16 (over y, x), tp: 16 (over z, core).
Axes of the slice: x: 4, y: 4, z: 8, core: 2. Of those that a mesh axis runs over, the one named last changes fastest.
Arguments:
- normed_inputs: bfloat16 [16384, 4096], P('fs', 'tp'), may hold values from -6 to 6
- query_upstream: bfloat16 [16384, 4096], P('fs', 'tp'), may hold values from -0.0625 to 0.0625
- key_upstream: bfloat16 [16384, 1024], P('fs', 'tp'), may hold values from -0.046875 to 0.046875
- head_outputs: bfloat16 [16384, 4096], P('fs', 'tp'), may hold values from -6 to 6
- branch_upstream: bfloat16 [16384, 4096], P('fs', 'tp'), may hold values from -0.0625 to 0.0625
- query_master: float32 [4096, 4096], P('fs', 'tp'), may hold values from -0.09375 to 0.09375
- key_master: float32 [4096, 1024], P('fs', 'tp'), may hold values from -0.09375 to 0.09375
- branch_master: float32 [4096, 4096], P('fs', 'tp'), may hold values from -0.09375 to 0.09375
- query_basis: bfloat16 [4096, 128], replicated, may hold values from -0.09375 to 0.09375
- key_basis: bfloat16 [4096, 128], replicated, may hold values from -0.09375 to 0.09375
- branch_basis: bfloat16 [4096, 128], replicated, may hold values from -0.09375 to 0.09375
- query_first: float32 [128, 4096], P(None, 'tp'), may hold values from -0.75 to 0.75
- query_second: float32 [128, 4096], P(None, 'tp'), may hold values from 0.001 to 0.02
- key_first: float32 [128, 1024], P(None, 'tp'), may hold values from -0.75 to 0.75
- key_second: float32 [128, 1024], P(None, 'tp'), may hold values from 0.001 to 0.02
- branch_first: float32 [4096, 128], P('fs'), may hold values from -0.75 to 0.75
- branch_second: float32 [4096, 128], P('fs'), may hold values from 0.001 to 0.02
Outputs:
- query_step: float32 [4096, 4096], P('fs', 'tp')
- key_step: float32 [4096, 1024], P('fs', 'tp')
- branch_step: float32 [4096, 4096], P('fs', 'tp')
- query_updated: float32 [4096, 4096], P('fs', 'tp')
- key_updated: float32 [4096, 1024], P('fs', 'tp')
- branch_updated: float32 [4096, 4096], P('fs', 'tp')
- query_copy: bfloat16 [4096, 4096], P(None, 'tp')
- key_copy: bfloat16 [4096, 1024], P(None, 'tp')
- branch_copy: bfloat16 [4096, 4096], P(None, 'tp')
- query_first_new: float32 [128, 4096], P(None, 'tp')
- query_second_new: float32 [128, 4096], P(None, 'tp')
- key_first_new: float32 [128, 1024], P(None, 'tp')
- key_second_new: float32 [128, 1024], P(None, 'tp')
- branch_first_new: float32 [4096, 128], P('fs')
- branch_second_new: float32 [4096, 128], P('fs')
The draws below stay inside these ranges and needn't reach their ends.
All inputs are finite; a program needn't handle non-finite values.
Results may differ from the reference program's by a relative error of at most 0.001.
Values may be sent and summed in bfloat16 or wider, within the bound.
A program may use at most 128 MiB of HBM per device.

```python
import math
import jax
import jax.numpy as jnp
from jax import lax

D = 4096
RANK = 128
HW = 4096
KW = 1024
TOKENS = 16384


def strengthened(drawn, own_key, source, target, blocks, factor):
    def block_of(axis_at):
        return (jnp.arange(drawn.shape[axis_at]) // (drawn.shape[axis_at] // blocks)).reshape((-1,) + (1,) * (drawn.ndim - 1 - axis_at))

    near = jax.random.permutation(own_key, blocks)[block_of(target)]
    other_side = (block_of(target) + blocks // 2) % blocks
    return jnp.where((block_of(source) == near) | (block_of(source) == other_side), factor * drawn, drawn)


def steps_of(key, extent, split, least, top_value):
    def one(position, blocks):
        draws = jax.random.uniform(jax.random.fold_in(jax.random.fold_in(key, 6), position), (blocks,), jnp.float32, least / len(split), top_value / len(split))
        return jnp.repeat(jnp.exp(draws), extent[position] // blocks).reshape((-1,) + (1,) * (len(extent) - position - 1))

    loudness = one(*split[0])
    for cut in split[1:]:
        loudness = loudness * one(*cut)
    return loudness


def centred(rng, extent, width, most, cuts=(), held_as=jnp.bfloat16):
    values = width * jax.random.normal(rng, extent, jnp.float32)
    if cuts:
        values = values * steps_of(rng, extent, cuts, -0.22, 0.18)
    return jnp.clip(values, -most, most).astype(held_as)


def gaussian_with(stream_key, dims, spread, limit, shards, heavy, kind=jnp.bfloat16):
    drawn = spread * jax.random.normal(stream_key, dims, jnp.float32)
    if shards:
        drawn = drawn * steps_of(stream_key, dims, shards, -0.22, 0.18)
    return jnp.clip(strengthened(drawn, jax.random.fold_in(stream_key, 3), *heavy), -limit, limit).astype(kind)


def setup_inputs(seed: int = 0) -> dict:
    key_list = jax.random.split(jax.random.key(seed), 18)
    normed_inputs = centred(key_list[0], (TOKENS, D), 1.0, 6.0, ((0, 16), (1, 16)))
    query_upstream = gaussian_with(key_list[1], (TOKENS, HW), TOKENS ** -0.5, 0.0625, ((0, 16), (1, 16)), (0, 1, 16, 2.0))
    key_upstream = centred(key_list[2], (TOKENS, KW), TOKENS ** -0.5, 0.046875, ((0, 16), (1, 16)))
    head_outputs = centred(key_list[3], (TOKENS, HW), 1.0, 6.0, ((0, 16), (1, 16)))
    branch_upstream = gaussian_with(key_list[4], (TOKENS, D), TOKENS ** -0.5, 0.0625, ((0, 16), (1, 16)), (0, 1, 16, 2.0))
    query_master = centred(key_list[5], (D, HW), D ** -0.5, 0.09375, ((0, 16), (1, 16)), jnp.float32)
    key_master = centred(key_list[6], (D, KW), D ** -0.5, 0.09375, ((0, 16), (1, 16)), jnp.float32)
    branch_master = centred(key_list[7], (HW, D), HW ** -0.5, 0.09375, ((0, 16), (1, 16)), jnp.float32)
    query_basis = centred(key_list[8], (D, RANK), D ** -0.5, 0.09375)
    key_basis = centred(key_list[9], (D, RANK), D ** -0.5, 0.09375)
    branch_basis = centred(key_list[10], (D, RANK), D ** -0.5, 0.09375)
    query_first = centred(key_list[11], (RANK, HW), 0.05, 0.75, ((1, 16),), jnp.float32)
    query_second = jnp.clip(jnp.exp(math.log(0.02) - 2.9957322 * jax.random.uniform(key_list[12], (RANK, HW), jnp.float32) ** steps_of(key_list[12], (RANK, HW), ((1, 16),), -0.2, 0.2)), 0.001, 0.02)
    key_first = centred(key_list[13], (RANK, KW), 0.05, 0.75, ((1, 16),), jnp.float32)
    key_second = jnp.clip(jnp.exp(math.log(0.02) - 2.9957322 * jax.random.uniform(key_list[14], (RANK, KW), jnp.float32) ** steps_of(key_list[14], (RANK, KW), ((1, 16),), -0.2, 0.2)), 0.001, 0.02)
    branch_first = centred(key_list[15], (HW, RANK), 0.05, 0.75, ((0, 16),), jnp.float32)
    branch_second = jnp.clip(jnp.exp(math.log(0.02) - 2.9957322 * jax.random.uniform(key_list[16], (HW, RANK), jnp.float32) ** steps_of(key_list[16], (HW, RANK), ((0, 16),), -0.2, 0.2)), 0.001, 0.02)
    return {"normed_inputs": normed_inputs, "query_upstream": query_upstream, "key_upstream": key_upstream, "head_outputs": head_outputs, "branch_upstream": branch_upstream, "query_master": query_master, "key_master": key_master, "branch_master": branch_master, "query_basis": query_basis, "key_basis": key_basis, "branch_basis": branch_basis, "query_first": query_first, "query_second": query_second, "key_first": key_first, "key_second": key_second, "branch_first": branch_first, "branch_second": branch_second}


LEARN = 0.02
BETA_ONE = 0.9
BETA_TWO = 0.95
ADAM_EPS = 1e-08
CLIP_RMS = 0.5

def moments(first, second, low, clip):
    scaled = clip * low
    first_new = BETA_ONE * first + (1.0 - BETA_ONE) * scaled
    second_new = BETA_TWO * second + (1.0 - BETA_TWO) * scaled * scaled
    return (first_new, second_new, first_new / (jnp.sqrt(second_new) + ADAM_EPS))

def reference(normed_inputs, query_upstream, key_upstream, head_outputs, branch_upstream, query_master, key_master, branch_master, query_basis, key_basis, branch_basis, query_first, query_second, key_first, key_second, branch_first, branch_second):
    exact = lax.Precision.HIGHEST
    query_grad = jnp.dot(normed_inputs.T, query_upstream, preferred_element_type=jnp.float32)
    key_grad = jnp.dot(normed_inputs.T, key_upstream, preferred_element_type=jnp.float32)
    branch_grad = jnp.dot(head_outputs.T, branch_upstream, preferred_element_type=jnp.float32)
    query_low = jnp.dot(query_basis.astype(jnp.float32).T, query_grad, precision=exact)
    key_low = jnp.dot(key_basis.astype(jnp.float32).T, key_grad, precision=exact)
    branch_low = jnp.dot(branch_grad, branch_basis.astype(jnp.float32), precision=exact)
    total = jnp.sum(query_low * query_low) + jnp.sum(key_low * key_low) + jnp.sum(branch_low * branch_low)
    entries = query_low.size + key_low.size + branch_low.size
    rms_value = jnp.sqrt(total / float(entries))
    clip = 1.0 / jnp.maximum(1.0, rms_value / CLIP_RMS)
    q_first, q_second, q_dir = moments(query_first, query_second, query_low, clip)
    k_first, k_second, k_dir = moments(key_first, key_second, key_low, clip)
    b_first, b_second, b_dir = moments(branch_first, branch_second, branch_low, clip)
    query_step = jnp.dot(query_basis.astype(jnp.float32), q_dir, precision=exact)
    key_step = jnp.dot(key_basis.astype(jnp.float32), k_dir, precision=exact)
    branch_step = jnp.dot(b_dir, branch_basis.astype(jnp.float32).T, precision=exact)
    query_updated = query_master - LEARN * query_step
    key_updated = key_master - LEARN * key_step
    branch_updated = branch_master - LEARN * branch_step
    return (query_step, key_step, branch_step, query_updated, key_updated, branch_updated, query_updated.astype(jnp.bfloat16), key_updated.astype(jnp.bfloat16), branch_updated.astype(jnp.bfloat16), q_first, q_second, k_first, k_second, b_first, b_second)
```

```python
import functools

import jax
import jax.numpy as jnp
from jax import lax
from jax.experimental import pallas as pl
from jax.experimental.pallas import tpu as pltpu
from jax.sharding import Mesh
from jax.sharding import PartitionSpec as P

FS = ("fs_0", "fs_1")
TP = ("tp_0", "tp_1")
MESH = pl.DeviceIdType.MESH

LEARN = 0.02
BETA_ONE = 0.9
BETA_TWO = 0.95
ADAM_EPS = 1e-08
CLIP_RMS = 0.5

NY, NX, NZ, NC = 4, 4, 8, 2
NF, NT = NY * NX, NZ * NC
F32, BF16 = jnp.float32, jnp.bfloat16
REACH = {(0, 1): 4, (0, -1): 3, (1, 1): 3, (1, -1): 4}
AXES = {"y": "fs_0", "x": "fs_1", "z": "tp_0", "c": "tp_1"}


def dot(a, b, ca=1, cb=0):
    return lax.dot_general(a, b, (((ca,), (cb,)), ((), ())), preferred_element_type=F32)


def split(value):
    high = value.astype(BF16)
    return high, (value - high.astype(F32)).astype(BF16)


def moments(first, second, low, clip):
    scaled = clip * low
    first_new = BETA_ONE * first + (1.0 - BETA_ONE) * scaled
    second_new = BETA_TWO * second + (1.0 - BETA_TWO) * scaled * scaled
    return first_new, second_new, first_new / (jnp.sqrt(second_new) + ADAM_EPS)


class Gather:
    def __init__(self, buf, y, x, send, recv):
        self.buf, self.at, self.send, self.recv = buf, {"y": y, "x": x}, send, recv
        self.half = buf.shape[1] // 2
        self.sent = []

    def copy(self, h, kind, a, way, arriving):
        dims = ("x", "y") if h == 0 else ("y", "x")
        index = {"p1": 0, "f1": 2, "p2": 4, "f2": 12}[kind] + (0 if way == 1 else 1)
        if kind in ("p2", "f2"):
            index += 2 * (0, -1, 1, 2).index(a)
        passed = (0 if kind[0] == "p" else 1) + (1 if arriving else 0)
        off = (-way * passed, 0) if kind[1] == "1" else (a, -way * passed)
        pos = {d: lax.rem(self.at[d] + (o + 4), 4) for d, o in zip(dims, off)}
        block = pos["y"] * NX + pos["x"]
        start, size = h * self.half, self.half
        if kind[0] == "f":
            size //= 2
            start += 0 if way == 1 else size
        ref = self.buf.at[block, pl.ds(start, size)]
        dim = dims[int(kind[1]) - 1]
        return pltpu.make_async_remote_copy(
            src_ref=ref,
            dst_ref=ref,
            send_sem=self.send.at[h * 20 + index],
            recv_sem=self.recv.at[h * 20 + index],
            device_id={AXES[dim]: lax.rem(self.at[dim] + (way + 4), 4)},
            device_id_type=MESH,
        )

    def start(self, h, kind, a, way):
        self.copy(h, kind, a, way, False).start()
        self.sent.append((h, kind, a, way))

    def wait(self, h, kind, a, way):
        self.copy(h, kind, a, way, True).wait_recv()

    def both(self, h, a):
        for way in (1, -1):
            self.start(h, "p2", a, way)

    def step(self, n):
        for h in (0, 1):
            if n == 0:
                for way in (1, -1):
                    self.start(h, "p1", 0, way)
                self.both(h, 0)
            elif n == 1:
                for way in (1, -1):
                    self.wait(h, "p1", 0, way)
                    self.start(h, "f1", 0, way)
                    self.both(h, -way)
            elif n == 3:
                for way in (1, -1):
                    self.wait(h, "f1", 0, way)
                self.both(h, 2)
            elif n == 6:
                for a in (0, -1, 1, 2):
                    for way in (1, -1):
                        self.wait(h, "f2", a, way)
            else:
                for a in {2: (0,), 4: (-1, 1), 5: (2,)}[n]:
                    for way in (1, -1):
                        self.wait(h, "p2", a, way)
                        self.start(h, "f2", a, way)

    def finish(self):
        for m in self.sent:
            self.copy(*m, False).wait_send()


def exchange_kernel(
    x_hbm, uq_hbm, uk_hbm, h_hbm, ub_hbm, mq_hbm, mk_hbm, mb_hbm, bq_hbm, bk_hbm, bb_hbm,
    qf_hbm, qs_hbm, kf_hbm, ks_hbm, bf_hbm, bs_hbm,
    qc_out, kc_out, bc_out, lq_out, lk_out, lb_out, clip_out,
    xv, uv, uqv, ukv, hv, bqv, bkv, bbv, mkv, mbv, qf, qs, kf, ks, bf, bs,
    g, gb, s1, rr, ss, p2, hi, lo, s2, r2, g3, b3, s4, r4, oq, ok, qd, kd,
    lsem, dsend, drecv, zs, zr, as_, ar, fwds, fwdr, g1s, g1r, g2s, g2r, ps, pr, osem,
):
    y, x = lax.axis_index("fs_0"), lax.axis_index("fs_1")
    z, c = lax.axis_index("tp_0"), lax.axis_index("tp_1")
    f, t = y * NX + x, z * NC + c

    loads = []

    def load(src, dst):
        copy = pltpu.make_async_copy(src, dst, lsem.at[len(loads)])
        copy.start()
        loads.append(copy)
        return copy

    mine, other = pl.ds(c * 512, 512), pl.ds((1 - c) * 512, 512)
    gq0 = load(mq_hbm.at[:, pl.ds(0, 128)], g.at[f, pl.ds(0, 256)])
    gq1 = load(mq_hbm.at[:, pl.ds(128, 128)], g.at[f, pl.ds(256, 256)])
    gk = load(mk_hbm, mkv)
    first = [
        load(x_hbm.at[mine], xv.at[c]),
        load(ub_hbm.at[mine], uv.at[c]),
        load(bb_hbm.at[pl.ds(z * 512, 512)], bbv),
        load(bq_hbm, bqv),
        load(bk_hbm, bkv),
    ]
    second = [load(uq_hbm, uqv), load(uk_hbm, ukv), load(h_hbm, hv)]
    third = [
        load(a, b)
        for a, b in (
            (mb_hbm, mbv), (qf_hbm, qf), (qs_hbm, qs), (kf_hbm, kf), (ks_hbm, ks), (bf_hbm, bf), (bs_hbm, bs),
        )
    ]

    def fs_peer(d):
        p = lax.rem(f + d, NF)
        return p, {"fs_0": p // NX, "fs_1": lax.rem(p, NX)}

    def tp_peer(d):
        p = lax.rem(t + d, NT)
        return p, {"tp_0": p // NC, "tp_1": lax.rem(p, NC)}

    barrier = pltpu.get_barrier_semaphore()

    @pl.loop(1, 16)
    def _(d):
        pl.semaphore_signal(barrier, inc=1, device_id=fs_peer(d)[1], device_id_type=MESH)
        pl.semaphore_signal(barrier, inc=1, device_id=tp_peer(d)[1], device_id_type=MESH)

    pl.semaphore_wait(barrier, 30)

    def remote(src, dst, send, recv, to):
        return pltpu.make_async_remote_copy(
            src_ref=src, dst_ref=dst, send_sem=send, recv_sem=recv, device_id=to, device_id_type=MESH
        )

    partner = {"tp_1": 1 - c}
    swaps = [
        remote(x_hbm.at[other], xv.at[c], dsend.at[0], drecv.at[0], partner),
        remote(ub_hbm.at[other], uv.at[c], dsend.at[1], drecv.at[1], partner),
    ]
    for s in swaps:
        s.start()

    gk.wait()
    g[f, pl.ds(512, 128)] = jnp.concatenate([mkv[0:128], mkv[128:256]], axis=1)
    gq0.wait()
    gq1.wait()
    whole = Gather(g, y, x, g1s, g1r)
    whole.step(0)

    for a in first:
        a.wait()
    for s in swaps:
        s.wait_recv()
    za, zb = pl.ds(z * 512, 256), pl.ds(z * 512 + 256, 256)
    proj = (
        dot(xv[0], bqv[za]) + dot(xv[1], bqv[zb]),
        dot(xv[0], bkv[za]) + dot(xv[1], bkv[zb]),
        dot(uv[0], bbv[0:256]) + dot(uv[1], bbv[256:512]),
    )
    for i in range(3):
        for o in range(NZ):
            for h in (0, 1):
                at = (2 * o + h) * 32
                s1[o, h, i * 32 : i * 32 + 32] = proj[i][at : at + 32]

    def ring(table, h, way, s):
        index = (h * 2 + (0 if way == 1 else 1)) * 4 + s
        return table.at[index]

    def zmove(src, dst, sends, recvs, h, way, s):
        to = {"tp_0": lax.rem(z + (way + NZ), NZ)}
        return remote(src, dst, ring(sends, h, way, s), ring(recvs, h, way, s), to)

    lanes = [(h, way) for h in (0, 1) for way in (1, -1)]
    zsent = []
    for s in range(4):
        for h, way in lanes:
            reach = REACH[h, way]
            if s >= reach:
                continue
            owner = lax.rem(z + way * (reach - s) + NZ, NZ)
            if s == 0:
                src = s1.at[owner, h]
            else:
                zmove(src, ring(rr, h, way, s - 1), zs, zr, h, way, s - 1).wait_recv()
                src = ring(ss, h, way, s)
                src[...] = ring(rr, h, way, s - 1)[...] + s1[owner, h]
            zsent.append((src, ring(rr, h, way, s), zs, zr, h, way, s))
            zmove(*zsent[-1]).start()
        if s == 2:
            whole.step(1)
    whole.step(2)
    for h in (0, 1):
        total = s1[z, h]
        for way in (1, -1):
            last = REACH[h, way] - 1
            zmove(s1.at[z, h], ring(rr, h, way, last), zs, zr, h, way, last).wait_recv()
            total = total + ring(rr, h, way, last)[...]
        p2[c, z, h] = total

    def over(h, o, index):
        ref = p2.at[c, o, h]
        return remote(ref, ref, fwds.at[h * 8 + index], fwdr.at[h * 8 + index], partner)

    asent, osent = [], []

    def onward(h, o, index):
        over(h, o, index).start()
        osent.append((h, o, index))

    for s in range(5):
        for h, way in lanes:
            reach = REACH[h, way]
            if s > reach:
                continue
            o = lax.rem(z - way * s + NZ, NZ)
            ref = p2.at[c, o, h]
            if s > 0:
                zmove(ref, ref, as_, ar, h, way, s - 1).wait_recv()
            if s < reach:
                zmove(ref, ref, as_, ar, h, way, s).start()
                asent.append((ref, ref, as_, ar, h, way, s))
            if s > 0 or way == 1:
                onward(h, o, s if way == 1 else NZ - s)
        if s == 1:
            whole.step(3)
        if s == 3:
            whole.step(4)

    for a in second:
        a.wait()

    def spread(half):
        for i in range(3):
            value = p2[half, :, :, i * 32 : i * 32 + 32].reshape(512, 128)
            rows = pl.ds(half * 512, 512)
            hi[i, rows], lo[i, rows] = split(value)

    spread(c)
    for h in (0, 1):
        for index in range(NZ):
            o = lax.rem(z - index + NZ, NZ)
            ref = p2.at[1 - c, o, h]
            remote(ref, ref, fwds.at[h * 8 + index], fwdr.at[h * 8 + index], partner).wait_recv()
    spread(1 - c)

    uq, uk, hh = uqv[...], ukv[...], hv[...]
    low_q = dot(hi[0], uq, 0, 0) + dot(lo[0], uq, 0, 0)
    low_k = dot(hi[1], uk, 0, 0) + dot(lo[1], uk, 0, 0)
    low_b = dot(hh, hi[2], 0, 0) + dot(hh, lo[2], 0, 0)
    low_k = jnp.concatenate([low_k, jnp.zeros((128, 64), F32)], axis=1)
    for p in range(NF):
        s2[p, 0:8] = low_q[8 * p : 8 * p + 8, 0:128]
        s2[p, 8:16] = low_q[8 * p : 8 * p + 8, 128:256]
        s2[p, 16:24] = low_k[8 * p : 8 * p + 8]
        s2[p, 24:40] = low_b[16 * p : 16 * p + 16]

    def fs_all(src, dst, k, act):
        @pl.loop(1, 16)
        def _(d):
            p, to = fs_peer(d)
            act(remote(src(p), dst.at[f], ps.at[k, d], pr.at[k, d], to))

    def tp_all(src, dst, k, act):
        @pl.loop(1, 16)
        def _(d):
            _, to = tp_peer(d)
            act(remote(src, dst.at[t], ps.at[k, d], pr.at[k, d], to))

    def fs_arrive(dst, k):
        @pl.loop(1, 16)
        def _(d):
            p = lax.rem(f + NF - d, NF)
            remote(dst.at[p], dst.at[p], ps.at[k, d], pr.at[k, d], fs_peer(d)[1]).wait_recv()

    def tp_arrive(dst, k):
        @pl.loop(1, 16)
        def _(d):
            p = lax.rem(t + NT - d, NT)
            remote(dst.at[p], dst.at[p], ps.at[k, d], pr.at[k, d], tp_peer(d)[1]).wait_recv()

    begin = lambda m: m.start()
    left = lambda m: m.wait_send()
    fs_all(lambda p: s2.at[p], r2, 0, begin)
    r2[f] = s2[f]
    fs_arrive(r2, 0)
    piece = r2[0]
    for p in range(1, NF):
        piece = piece + r2[p]
    squares = piece * piece
    tile = squares[0:8]
    for i in range(1, 5):
        tile = tile + squares[8 * i : 8 * i + 8]
    b3[t, 0:16] = piece[24:40]
    b3[t, 16:24] = tile
    g3[f] = piece[0:24]
    tp_all(b3.at[t], b3, 1, begin)
    fs_all(lambda p: g3.at[f], g3, 2, begin)
    tp_arrive(b3, 1)
    tile = b3[0, 16:24]
    for i in range(1, NT):
        tile = tile + b3[i, 16:24]
    for i in range(NT):
        s4[i, 0:16] = b3[i, 0:16]
        s4[i, 16:24] = tile
    fs_all(lambda p: s4.at[p], r4, 3, begin)
    r4[f] = s4[f]
    fs_arrive(g3, 2)
    whole.step(5)
    fs_arrive(r4, 3)
    tile = r4[0, 16:24]
    for i in range(1, NF):
        tile = tile + r4[i, 16:24]
    total = jnp.sum(jnp.sum(tile, axis=0, keepdims=True), axis=1, keepdims=True)
    entries = 128 * (2 * 4096 + 1024)
    rms = jnp.sqrt(total / float(entries))
    clip = 1.0 / jnp.maximum(1.0, rms / CLIP_RMS)
    clip_out[...] = jnp.broadcast_to(clip, (8, 128))

    for a in third:
        a.wait()

    low_b = r4[:, 0:16].reshape(256, 128)
    lb_out[...] = low_b
    _, _, dir_b = moments(bf[...], bs[...], low_b, clip)
    dh, dl = split(dir_b)
    cols = bbv[pl.ds(c * 256, 256)]
    new_b = (mbv[...] - LEARN * (dot(dh, cols, 1, 1) + dot(dl, cols, 1, 1))).astype(BF16)
    gb[f, 0:256] = new_b[:, 0:128]
    gb[f, 256:512] = new_b[:, 128:256]
    branch = Gather(gb, y, x, g2s, g2r)
    branch.step(0)

    low_q = jnp.concatenate([g3[:, 0:8].reshape(128, 128), g3[:, 8:16].reshape(128, 128)], axis=1)
    low_k = g3[:, 16:24].reshape(128, 128)[:, 0:64]
    lq_out[...] = low_q
    lk_out[...] = low_k
    _, _, dir_q = moments(qf[...], qs[...], low_q, clip)
    _, _, dir_k = moments(kf[...], ks[...], low_k, clip)
    qd[0], qd[1] = split(dir_q)
    kd[0], kd[1] = split(dir_k)
    whole.step(6)

    def own_columns(j):
        rows = pl.ds(pl.multiple_of(j * 256, 256), 256)
        bq, bk = bqv[rows], bkv[rows]
        step = LEARN * (dot(bq, qd[0]) + dot(bq, qd[1]))
        oq[rows, 0:128] = (g[j, 0:256] - step[:, 0:128]).astype(BF16)
        oq[rows, 128:256] = (g[j, 256:512] - step[:, 128:256]).astype(BF16)
        step = LEARN * (dot(bk, kd[0]) + dot(bk, kd[1]))
        pair = g[j, 512:640]
        ok[rows] = (jnp.concatenate([pair[:, 0:64], pair[:, 64:128]], axis=0) - step).astype(BF16)

    def put(j, act):
        rows = pl.ds(pl.multiple_of(j * 1024, 1024), 1024)
        act(pltpu.make_async_copy(oq.at[rows], qc_out.at[rows], osem.at[0, j]))
        act(pltpu.make_async_copy(ok.at[rows], kc_out.at[rows], osem.at[1, j]))

    for quarter in range(4):
        pl.loop(quarter * 4, quarter * 4 + 4)(own_columns)
        put(quarter, begin)
        branch.step(quarter + 1)
    branch.step(5)
    branch.step(6)

    def put_branch(act):
        @pl.loop(0, 16)
        def _(j):
            rows = pl.ds(pl.multiple_of(j * 256, 256), 256)
            for half in (0, 1):
                src = gb.at[j, pl.ds(half * 256, 256)]
                act(pltpu.make_async_copy(src, bc_out.at[rows, pl.ds(half * 128, 128)], osem.at[2 + half, j]))

    put_branch(begin)

    for s in swaps:
        s.wait_send()
    for m in zsent + asent:
        zmove(*m).wait_send()
    for m in osent:
        over(*m).wait_send()
    fs_all(lambda p: s2.at[p], r2, 0, left)
    tp_all(b3.at[t], b3, 1, left)
    fs_all(lambda p: g3.at[f], g3, 2, left)
    fs_all(lambda p: s4.at[p], r4, 3, left)
    whole.finish()
    branch.finish()
    for quarter in range(4):
        put(quarter, lambda m: m.wait())
    put_branch(lambda m: m.wait())


def finish_kernel(
    mq, mk, mb, bq, bk, bb, qf, qs, kf, ks, bf, bs, lq, lk, lb, clip_ref,
    q_step, k_step, b_step, q_new, k_new, b_new, qf_new, qs_new, kf_new, ks_new, bf_new, bs_new,
    bqv, bkv, bbv, sem,
):
    f = lax.axis_index("fs_0") * NX + lax.axis_index("fs_1")
    t = lax.axis_index("tp_0") * NC + lax.axis_index("tp_1")
    copies = [
        pltpu.make_async_copy(src.at[pl.ds(at * 256, 256)], dst, sem.at[i])
        for i, (src, dst, at) in enumerate(((bq, bqv, f), (bk, bkv, f), (bb, bbv, t)))
    ]
    for copy in copies:
        copy.start()
    clip = clip_ref[0:1, 0:1]
    for copy in copies:
        copy.wait()

    def one(first, second, low, master, basis, first_out, second_out, step_out, new_out, branch):
        first_out[...], second_out[...], way = moments(first[...], second[...], low[...], clip)
        high, rest = split(way)
        if branch:
            step = dot(high, basis[...], 1, 1) + dot(rest, basis[...], 1, 1)
        else:
            step = dot(basis[...], high) + dot(basis[...], rest)
        step_out[...] = step
        new_out[...] = master[...] - LEARN * step

    one(qf, qs, lq, mq, bqv, qf_new, qs_new, q_step, q_new, False)
    one(kf, ks, lk, mk, bkv, kf_new, ks_new, k_step, k_new, False)
    one(bf, bs, lb, mb, bbv, bf_new, bs_new, b_step, b_new, True)


def per_device(*args):
    (_, _, _, _, _, mq, mk, mb, bq, bk, bb, qf, qs, kf, ks, bf, bs) = args
    shape = jax.ShapeDtypeStruct
    hbm = pl.BlockSpec(memory_space=pl.ANY)
    vmem = pl.BlockSpec(memory_space=pltpu.VMEM)
    v, dma = pltpu.VMEM, pltpu.SemaphoreType.DMA
    qc, kc, bc, lq, lk, lb, clip = pl.pallas_call(
        exchange_kernel,
        name="exchange",
        out_shape=(
            shape((4096, 256), BF16),
            shape((4096, 64), BF16),
            shape((4096, 256), BF16),
            shape((128, 256), F32),
            shape((128, 64), F32),
            shape((256, 128), F32),
            shape((8, 128), F32),
        ),
        in_specs=[hbm] * 17,
        out_specs=(hbm, hbm, hbm, vmem, vmem, vmem, vmem),
        scratch_shapes=[
            v((2, 512, 256), BF16), v((2, 512, 256), BF16), v((1024, 256), BF16), v((1024, 64), BF16),
            v((1024, 256), BF16), v((4096, 128), BF16), v((4096, 128), BF16), v((512, 128), BF16),
            v((256, 64), F32), v((256, 256), F32), v((128, 256), F32), v((128, 256), F32),
            v((128, 64), F32), v((128, 64), F32), v((256, 128), F32), v((256, 128), F32),
            v((16, 640, 128), F32), v((16, 512, 128), BF16), v((8, 2, 96, 128), F32),
            v((16, 96, 128), F32), v((16, 96, 128), F32), v((2, 8, 2, 96, 128), F32),
            v((3, 1024, 128), BF16), v((3, 1024, 128), BF16), v((16, 40, 128), F32), v((16, 40, 128), F32),
            v((16, 24, 128), F32), v((16, 24, 128), F32), v((16, 24, 128), F32), v((16, 24, 128), F32),
            v((4096, 256), BF16), v((4096, 64), BF16), v((2, 128, 256), BF16), v((2, 128, 64), BF16),
            dma((18,)), dma((2,)), dma((2,)), dma((16,)), dma((16,)), dma((16,)), dma((16,)),
            dma((16,)), dma((16,)), dma((40,)), dma((40,)), dma((40,)), dma((40,)),
            dma((4, 16)), dma((4, 16)), dma((4, 16)),
        ],
        compiler_params=pltpu.CompilerParams(
            collective_id=0, has_side_effects=True, vmem_limit_bytes=56 * 2**20
        ),
    )(*args)
    qst, kst, bst, qu, ku, bu, qf2, qs2, kf2, ks2, bf2, bs2 = pl.pallas_call(
        finish_kernel,
        name="finish",
        out_shape=tuple(
            shape(a.shape, F32) for a in (mq, mk, mb, mq, mk, mb, qf, qs, kf, ks, bf, bs)
        ),
        in_specs=[vmem] * 3 + [hbm] * 3 + [vmem] * 10,
        out_specs=(vmem,) * 12,
        scratch_shapes=[v((256, 128), BF16)] * 3 + [dma((3,))],
    )(mq, mk, mb, bq, bk, bb, qf, qs, kf, ks, bf, bs, lq, lk, lb, clip)
    return (qst, kst, bst, qu, ku, bu, qc, kc, bc, qf2, qs2, kf2, ks2, bf2, bs2)


def solution(mesh):
    finer = Mesh(mesh.devices.reshape(NY, NX, NZ, NC), FS + TP)
    fs_tp, cols, rows = P(FS, TP), P(None, TP), P(FS, None)
    return jax.shard_map(
        per_device,
        mesh=finer,
        in_specs=(fs_tp,) * 8 + (P(),) * 3 + (cols,) * 4 + (rows,) * 2,
        out_specs=(fs_tp,) * 6 + (cols,) * 7 + (rows,) * 2,
        check_vma=False,
    )
```

```python
import functools

import jax
import jax.numpy as jnp
from jax import lax
from jax.experimental import pallas as pl
from jax.experimental.pallas import tpu as pltpu
from jax.sharding import Mesh
from jax.sharding import PartitionSpec as P

FS = ("fs_0", "fs_1")
TP = ("tp_0", "tp_1")
MESH = pl.DeviceIdType.MESH

LEARN = 0.02
BETA_ONE = 0.9
BETA_TWO = 0.95
ADAM_EPS = 1e-08
CLIP_RMS = 0.5

NY, NX, NZ, NC = 4, 4, 8, 2
NF, NT = NY * NX, NZ * NC
F32, BF16 = jnp.float32, jnp.bfloat16
NH = 4
PARTS = tuple(range(NH))
REACH = {(h, way): 4 if (h % 2 == 0) == (way == 1) else 3 for h in PARTS for way in (1, -1)}
AXES = {"y": "fs_0", "x": "fs_1", "z": "tp_0", "c": "tp_1"}


def dot(a, b, ca=1, cb=0):
    return lax.dot_general(a, b, (((ca,), (cb,)), ((), ())), preferred_element_type=F32)


def split(value):
    high = value.astype(BF16)
    return high, (value - high.astype(F32)).astype(BF16)


def moments(first, second, low, clip):
    scaled = clip * low
    first_new = BETA_ONE * first + (1.0 - BETA_ONE) * scaled
    second_new = BETA_TWO * second + (1.0 - BETA_TWO) * scaled * scaled
    return first_new, second_new, first_new / (jnp.sqrt(second_new) + ADAM_EPS)


class Gather:
    def __init__(self, buf, y, x, send, recv):
        self.buf, self.at, self.send, self.recv = buf, {"y": y, "x": x}, send, recv
        self.half = buf.shape[1] // 2
        self.sent = []

    def copy(self, h, kind, a, way, arriving):
        dims = ("x", "y") if h == 0 else ("y", "x")
        index = {"p1": 0, "f1": 2, "p2": 4, "f2": 12}[kind] + (0 if way == 1 else 1)
        if kind in ("p2", "f2"):
            index += 2 * (0, -1, 1, 2).index(a)
        passed = (0 if kind[0] == "p" else 1) + (1 if arriving else 0)
        off = (-way * passed, 0) if kind[1] == "1" else (a, -way * passed)
        pos = {d: lax.rem(self.at[d] + (o + 4), 4) for d, o in zip(dims, off)}
        block = pos["y"] * NX + pos["x"]
        start, size = h * self.half, self.half
        if kind[0] == "f":
            size //= 2
            start += 0 if way == 1 else size
        ref = self.buf.at[block, pl.ds(start, size)]
        dim = dims[int(kind[1]) - 1]
        return pltpu.make_async_remote_copy(
            src_ref=ref,
            dst_ref=ref,
            send_sem=self.send.at[h * 20 + index],
            recv_sem=self.recv.at[h * 20 + index],
            device_id={AXES[dim]: lax.rem(self.at[dim] + (way + 4), 4)},
            device_id_type=MESH,
        )

    def start(self, h, kind, a, way):
        self.copy(h, kind, a, way, False).start()
        self.sent.append((h, kind, a, way))

    def wait(self, h, kind, a, way):
        self.copy(h, kind, a, way, True).wait_recv()

    def both(self, h, a):
        for way in (1, -1):
            self.start(h, "p2", a, way)

    def step(self, n):
        ways, halves = (1, -1), (0, 1)
        every = [(h, way) for h in halves for way in ways]
        if n == 0:
            for h, way in every:
                self.start(h, "p1", 0, way)
            for h in halves:
                self.both(h, 0)
        elif n == 1:
            for h, way in every:
                self.wait(h, "p1", 0, way)
                self.start(h, "f1", 0, way)
            for h, way in every:
                self.both(h, -way)
        elif n == 3:
            for h in halves:
                for way in ways:
                    self.wait(h, "f1", 0, way)
                self.both(h, 2)
        elif n == 6:
            for a in (0, -1, 1, 2):
                for h, way in every:
                    self.wait(h, "f2", a, way)
        else:
            for a in {2: (0,), 4: (-1, 1), 5: (2,)}[n]:
                for h, way in every:
                    self.wait(h, "p2", a, way)
                    self.start(h, "f2", a, way)

    def finish(self):
        for m in self.sent:
            self.copy(*m, False).wait_send()


def exchange_kernel(
    x_hbm, uq_hbm, uk_hbm, h_hbm, ub_hbm, mq_hbm, mk_hbm, mb_hbm, bq_hbm, bk_hbm, bb_hbm,
    qf_hbm, qs_hbm, kf_hbm, ks_hbm, bf_hbm, bs_hbm,
    oq, ok, bc_out, lq_out, lk_out, lb_out, clip_out,
    xv, uv, uqv, ukv, hv, bqv, bkv, bbv, mbv, qf, qs, kf, ks, bf, bs,
    g, gb, s1, rr, ss, p2, hi, lo, s2, r2, g3, b3, s4, r4, qd, kd,
    lsem, dsend, drecv, zs, zr, as_, ar, fwds, fwdr, g1s, g1r, g2s, g2r, ps, pr,
):
    y, x = lax.axis_index("fs_0"), lax.axis_index("fs_1")
    z, c = lax.axis_index("tp_0"), lax.axis_index("tp_1")
    f, t = y * NX + x, z * NC + c

    loads = []

    def load(src, dst):
        copy = pltpu.make_async_copy(src, dst, lsem.at[len(loads)])
        copy.start()
        loads.append(copy)
        return copy

    mine, other = pl.ds(c * 512, 512), pl.ds((1 - c) * 512, 512)
    gq0 = load(mq_hbm.at[:, pl.ds(0, 128)], g.at[f, pl.ds(0, 256)])
    gq1 = load(mq_hbm.at[:, pl.ds(128, 128)], g.at[f, pl.ds(256, 256)])
    gk0 = load(mk_hbm.at[:, pl.ds(0, 128)], g.at[f, pl.ds(512, 64)])
    gk1 = load(mk_hbm.at[:, pl.ds(128, 128)], g.at[f, pl.ds(576, 64)])
    first = [
        load(x_hbm.at[mine], xv.at[c]),
        load(ub_hbm.at[mine], uv.at[c]),
        load(bb_hbm.at[pl.ds(z * 512, 512)], bbv),
        load(bq_hbm, bqv),
        load(bk_hbm, bkv),
    ]
    second = [load(uq_hbm, uqv), load(uk_hbm, ukv), load(h_hbm, hv)]
    third = [
        load(a, b)
        for a, b in (
            (mb_hbm, mbv), (qf_hbm, qf), (qs_hbm, qs), (kf_hbm, kf), (ks_hbm, ks), (bf_hbm, bf), (bs_hbm, bs),
        )
    ]

    def fs_peer(d):
        p = lax.rem(f + d, NF)
        return p, {"fs_0": p // NX, "fs_1": lax.rem(p, NX)}

    def tp_peer(d):
        p = lax.rem(t + d, NT)
        return p, {"tp_0": p // NC, "tp_1": lax.rem(p, NC)}

    barrier = pltpu.get_barrier_semaphore()

    @pl.loop(1, 16)
    def _(d):
        pl.semaphore_signal(barrier, inc=1, device_id=fs_peer(d)[1], device_id_type=MESH)
        pl.semaphore_signal(barrier, inc=1, device_id=tp_peer(d)[1], device_id_type=MESH)

    pl.semaphore_wait(barrier, 30)

    def remote(src, dst, send, recv, to):
        return pltpu.make_async_remote_copy(
            src_ref=src, dst_ref=dst, send_sem=send, recv_sem=recv, device_id=to, device_id_type=MESH
        )

    partner = {"tp_1": 1 - c}
    swaps = [
        remote(x_hbm.at[other], xv.at[c], dsend.at[0], drecv.at[0], partner),
        remote(ub_hbm.at[other], uv.at[c], dsend.at[1], drecv.at[1], partner),
    ]
    for s in swaps:
        s.start()
    ends = [s.wait_send for s in swaps]

    for a in (gq0, gq1, gk0, gk1):
        a.wait()
    whole = Gather(g, y, x, g1s, g1r)
    whole.step(0)

    for a in first:
        a.wait()
    for s in swaps:
        s.wait_recv()
    za, zb = pl.ds(z * 512, 256), pl.ds(z * 512 + 256, 256)
    proj = (
        dot(xv[0], bqv[za]) + dot(xv[1], bqv[zb]),
        dot(xv[0], bkv[za]) + dot(xv[1], bkv[zb]),
        dot(uv[0], bbv[0:256]) + dot(uv[1], bbv[256:512]),
    )
    for i in range(3):
        for o in range(NZ):
            for h in PARTS:
                at = (NH * o + h) * 16
                s1[o, h, i * 16 : i * 16 + 16] = proj[i][at : at + 16]

    def ring(table, h, way, s):
        index = (h * 2 + (0 if way == 1 else 1)) * 4 + s
        return table.at[index]

    def zmove(src, dst, sends, recvs, h, way, s):
        to = {"tp_0": lax.rem(z + (way + NZ), NZ)}
        return remote(src, dst, ring(sends, h, way, s), ring(recvs, h, way, s), to)

    lanes = [(h, way) for h in PARTS for way in (1, -1)]
    for s in range(4):
        for h, way in lanes:
            reach = REACH[h, way]
            if s >= reach:
                continue
            owner = lax.rem(z + way * (reach - s) + NZ, NZ)
            if s == 0:
                src = s1.at[owner, h]
            else:
                zmove(src, ring(rr, h, way, s - 1), zs, zr, h, way, s - 1).wait_recv()
                src = ring(ss, h, way, s)
                src[...] = ring(rr, h, way, s - 1)[...] + s1[owner, h]
            move = zmove(src, ring(rr, h, way, s), zs, zr, h, way, s)
            move.start()
            ends.append(move.wait_send)
        if s == 2:
            whole.step(1)
    whole.step(2)

    def onward(h, o, index):
        ref = p2.at[c, o, h]
        move = remote(ref, ref, fwds.at[h * 8 + index], fwdr.at[h * 8 + index], partner)
        move.start()
        ends.append(move.wait_send)

    def along(h, o, way, s):
        ref = p2.at[c, o, h]
        move = zmove(ref, ref, as_, ar, h, way, s)
        move.start()
        ends.append(move.wait_send)

    for h in PARTS:
        total = s1[z, h]
        for way in (1, -1):
            last = REACH[h, way] - 1
            zmove(s1.at[z, h], ring(rr, h, way, last), zs, zr, h, way, last).wait_recv()
            total = total + ring(rr, h, way, last)[...]
        p2[c, z, h] = total
        for way in (1, -1):
            along(h, z, way, 0)
        onward(h, z, 0)
    for s in range(1, 5):
        for h, way in lanes:
            if s > REACH[h, way]:
                continue
            o = lax.rem(z - way * s + NZ, NZ)
            ref = p2.at[c, o, h]
            zmove(ref, ref, as_, ar, h, way, s - 1).wait_recv()
            if s < REACH[h, way]:
                along(h, o, way, s)
            onward(h, o, s if way == 1 else NZ - s)
        if s == 1:
            whole.step(3)
        if s == 3:
            whole.step(4)

    for a in second:
        a.wait()

    def spread(half):
        for i in range(3):
            value = p2[half, :, :, i * 16 : i * 16 + 16].reshape(512, 128)
            rows = pl.ds(half * 512, 512)
            hi[i, rows], lo[i, rows] = split(value)

    spread(c)
    for h in PARTS:
        for index in range(NZ):
            o = lax.rem(z - index + NZ, NZ)
            ref = p2.at[1 - c, o, h]
            remote(ref, ref, fwds.at[h * 8 + index], fwdr.at[h * 8 + index], partner).wait_recv()
    spread(1 - c)

    uq, uk, hh = uqv[...], ukv[...], hv[...]
    low_q = dot(hi[0], uq, 0, 0) + dot(lo[0], uq, 0, 0)
    low_k = dot(uk, hi[1]) + dot(uk, lo[1])
    low_b = dot(hh, hi[2], 0, 0) + dot(hh, lo[2], 0, 0)
    for p in range(NF):
        s2[p, 0:8] = low_q[8 * p : 8 * p + 8, 0:128]
        s2[p, 8:16] = low_q[8 * p : 8 * p + 8, 128:256]
        s2[p, 16:20] = low_k[4 * p : 4 * p + 4]
        s2[p, 20:24] = jnp.zeros((4, 128), F32)
        s2[p, 24:40] = low_b[16 * p : 16 * p + 16]

    def fs_all(src, dst, k, act):
        @pl.loop(1, 16)
        def _(d):
            p, to = fs_peer(d)
            act(remote(src(p), dst.at[f], ps.at[k, d], pr.at[k, d], to))

    def tp_all(src, dst, k, act):
        @pl.loop(1, 16)
        def _(d):
            _, to = tp_peer(d)
            act(remote(src, dst.at[t], ps.at[k, d], pr.at[k, d], to))

    def fs_arrive(dst, k):
        @pl.loop(1, 16)
        def _(d):
            p = lax.rem(f + NF - d, NF)
            remote(dst.at[p], dst.at[p], ps.at[k, d], pr.at[k, d], fs_peer(d)[1]).wait_recv()

    def tp_arrive(dst, k):
        @pl.loop(1, 16)
        def _(d):
            p = lax.rem(t + NT - d, NT)
            remote(dst.at[p], dst.at[p], ps.at[k, d], pr.at[k, d], tp_peer(d)[1]).wait_recv()

    begin = lambda m: m.start()
    left = lambda m: m.wait_send()
    fs_all(lambda p: s2.at[p], r2, 0, begin)
    ends.append(lambda: fs_all(lambda p: s2.at[p], r2, 0, left))
    r2[f] = s2[f]
    fs_arrive(r2, 0)
    piece = r2[0]
    for p in range(1, NF):
        piece = piece + r2[p]
    squares = piece * piece
    tile = squares[0:8]
    for i in range(1, 5):
        tile = tile + squares[8 * i : 8 * i + 8]
    b3[t, 0:16] = piece[24:40]
    b3[t, 16:24] = tile
    g3[f] = piece[0:24]
    tp_all(b3.at[t], b3, 1, begin)
    fs_all(lambda p: g3.at[f], g3, 2, begin)
    ends.append(lambda: tp_all(b3.at[t], b3, 1, left))
    ends.append(lambda: fs_all(lambda p: g3.at[f], g3, 2, left))
    tp_arrive(b3, 1)
    tile = b3[0, 16:24]
    for i in range(1, NT):
        tile = tile + b3[i, 16:24]
    for i in range(NT):
        s4[i, 0:16] = b3[i, 0:16]
        s4[i, 16:24] = tile
    fs_all(lambda p: s4.at[p], r4, 3, begin)
    ends.append(lambda: fs_all(lambda p: s4.at[p], r4, 3, left))
    r4[f] = s4[f]
    fs_arrive(g3, 2)
    whole.step(5)
    fs_arrive(r4, 3)
    tile = r4[0, 16:24]
    for i in range(1, NF):
        tile = tile + r4[i, 16:24]
    total = jnp.sum(jnp.sum(tile, axis=0, keepdims=True), axis=1, keepdims=True)
    entries = 128 * (2 * 4096 + 1024)
    rms = jnp.sqrt(total / float(entries))
    clip = 1.0 / jnp.maximum(1.0, rms / CLIP_RMS)
    clip_out[...] = jnp.broadcast_to(clip, (8, 128))

    for a in third:
        a.wait()

    low_b = r4[:, 0:16].reshape(256, 128)
    lb_out[...] = low_b
    _, _, dir_b = moments(bf[...], bs[...], low_b, clip)
    dh, dl = split(dir_b)
    cols = bbv[pl.ds(c * 256, 256)]
    new_b = (mbv[...] - LEARN * (dot(dh, cols, 1, 1) + dot(dl, cols, 1, 1))).astype(BF16)
    gb[f, 0:256] = new_b[:, 0:128]
    gb[f, 256:512] = new_b[:, 128:256]
    branch = Gather(gb, y, x, g2s, g2r)
    branch.step(0)

    low_q = jnp.concatenate([g3[:, 0:8].reshape(128, 128), g3[:, 8:16].reshape(128, 128)], axis=1)
    lq_out[...] = low_q
    for p in range(NF):
        lk_out[4 * p : 4 * p + 4] = g3[p, 16:20]
    low_k = lk_out[...]
    _, _, dir_q = moments(qf[...], qs[...], low_q, clip)
    _, _, dir_k = moments(kf[...], ks[...], low_k, clip)
    qd[0], qd[1] = split(dir_q)
    kd[0], kd[1] = split(dir_k)
    whole.step(6)

    def own_columns(j):
        rows = pl.ds(pl.multiple_of(j * 256, 256), 256)
        bq, bk = bqv[rows], bkv[rows]
        step = LEARN * (dot(bq, qd[0]) + dot(bq, qd[1]))
        oq[rows, 0:128] = (g[j, 0:256] - step[:, 0:128]).astype(BF16)
        oq[rows, 128:256] = (g[j, 256:512] - step[:, 128:256]).astype(BF16)
        step = LEARN * (dot(kd[0], bk, 1, 1) + dot(kd[1], bk, 1, 1))
        ok[:, rows] = (jnp.concatenate([g[j, 512:576], g[j, 576:640]], axis=1) - step).astype(BF16)

    done = 0
    for n, blocks in ((1, 3), (2, 2), (3, 1), (4, 2), (5, 4), (6, 4)):
        pl.loop(done, done + blocks)(own_columns)
        done += blocks
        branch.step(n)

    for m in ends:
        m()
    whole.finish()
    branch.finish()

    @pl.loop(0, 16)
    def _(j):
        rows = pl.ds(pl.multiple_of(j * 256, 256), 256)
        bc_out[rows, 0:128] = gb[j, 0:256]
        bc_out[rows, 128:256] = gb[j, 256:512]


def finish_kernel(
    mq, mk, mb, bq, bk, bb, qf, qs, kf, ks, bf, bs, lq, lk, lb, clip_ref, qc, kc, bc,
    q_step, k_step, b_step, q_new, k_new, b_new, qf_new, qs_new, kf_new, ks_new, bf_new, bs_new,
    qc_new, kc_new, bc_new, outsem,
):
    f = lax.axis_index("fs_0") * NX + lax.axis_index("fs_1")
    t = lax.axis_index("tp_0") * NC + lax.axis_index("tp_1")
    leaving = [
        pltpu.make_async_copy(src, dst, outsem.at[i])
        for i, (src, dst) in enumerate(((qc, qc_new), (kc, kc_new), (bc, bc_new)))
    ]
    for leave in leaving:
        leave.start()
    clip = clip_ref[0:1, 0:1]
    rows, cols = pl.ds(f * 256, 256), pl.ds(t * 256, 256)

    def one(first, second, low, master, basis, first_out, second_out, step_out, new_out, branch):
        first_out[...], second_out[...], way = moments(first[...], second[...], low[...], clip)
        high, rest = split(way)
        if branch:
            step = dot(high, basis, 1, 1) + dot(rest, basis, 1, 1)
        else:
            step = dot(basis, high) + dot(basis, rest)
        step_out[...] = step
        new_out[...] = master[...] - LEARN * step

    one(qf, qs, lq, mq, bq[rows], qf_new, qs_new, q_step, q_new, False)
    one(kf, ks, lk, mk, bk[rows], kf_new, ks_new, k_step, k_new, True)
    one(bf, bs, lb, mb, bb[cols], bf_new, bs_new, b_step, b_new, True)
    for leave in leaving:
        leave.wait()


def per_device(*args):
    args = tuple(a.T if i in (2, 6, 13, 14) else a for i, a in enumerate(args))
    (_, _, _, _, _, mq, mk, mb, bq, bk, bb, qf, qs, kf, ks, bf, bs) = args
    shape = jax.ShapeDtypeStruct
    hbm = pl.BlockSpec(memory_space=pltpu.HBM)
    vmem = pl.BlockSpec(memory_space=pltpu.VMEM)
    v, dma = pltpu.VMEM, pltpu.SemaphoreType.DMA
    qc, kc, bc, lq, lk, lb, clip = pl.pallas_call(
        exchange_kernel,
        name="exchange",
        out_shape=(
            shape((4096, 256), BF16),
            shape((64, 4096), BF16),
            shape((4096, 256), BF16),
            shape((128, 256), F32),
            shape((64, 128), F32),
            shape((256, 128), F32),
            shape((8, 128), F32),
        ),
        in_specs=[hbm] * 17,
        out_specs=(vmem,) * 7,
        scratch_shapes=[
            v((2, 512, 256), BF16), v((2, 512, 256), BF16), v((1024, 256), BF16), v((64, 1024), BF16),
            v((1024, 256), BF16), v((4096, 128), BF16), v((4096, 128), BF16), v((512, 128), BF16),
            v((256, 256), F32), v((128, 256), F32), v((128, 256), F32),
            v((64, 128), F32), v((64, 128), F32), v((256, 128), F32), v((256, 128), F32),
            v((16, 640, 128), F32), v((16, 512, 128), BF16), v((8, NH, 48, 128), F32),
            v((8 * NH, 48, 128), F32), v((8 * NH, 48, 128), F32), v((2, 8, NH, 48, 128), F32),
            v((3, 1024, 128), BF16), v((3, 1024, 128), BF16), v((16, 40, 128), F32), v((16, 40, 128), F32),
            v((16, 24, 128), F32), v((16, 24, 128), F32), v((16, 24, 128), F32), v((16, 24, 128), F32),
            v((2, 128, 256), BF16), v((2, 64, 128), BF16),
            dma((19,)), dma((2,)), dma((2,)), dma((8 * NH,)), dma((8 * NH,)), dma((8 * NH,)), dma((8 * NH,)),
            dma((8 * NH,)), dma((8 * NH,)), dma((40,)), dma((40,)), dma((40,)), dma((40,)),
            dma((4, 16)), dma((4, 16)),
        ],
        compiler_params=pltpu.CompilerParams(
            collective_id=0, has_side_effects=True, vmem_limit_bytes=28 * 2**20
        ),
    )(*(pltpu.with_memory_space_constraint(a, pltpu.HBM) for a in args))
    qst, kst, bst, qu, ku, bu, qf2, qs2, kf2, ks2, bf2, bs2, qc, kc, bc = pl.pallas_call(
        finish_kernel,
        name="finish",
        out_shape=tuple(
            shape(a.shape, F32) for a in (mq, mk, mb, mq, mk, mb, qf, qs, kf, ks, bf, bs)
        )
        + tuple(shape(a.shape, BF16) for a in (qc, kc, bc)),
        in_specs=[vmem] * 19,
        out_specs=(vmem,) * 12 + (hbm,) * 3,
        scratch_shapes=[dma((3,))],
        compiler_params=pltpu.CompilerParams(vmem_limit_bytes=20 * 2**20),
    )(mq, mk, mb, bq, bk, bb, qf, qs, kf, ks, bf, bs, lq, lk, lb, clip, qc, kc, bc)
    return (qst, kst.T, bst, qu, ku.T, bu, qc, kc.T, bc, qf2, qs2, kf2.T, ks2.T, bf2, bs2)


def solution(mesh):
    finer = Mesh(mesh.devices.reshape(NY, NX, NZ, NC), FS + TP)
    fs_tp, cols, rows = P(FS, TP), P(None, TP), P(FS, None)
    return jax.shard_map(
        per_device,
        mesh=finer,
        in_specs=(fs_tp,) * 8 + (P(),) * 3 + (cols,) * 4 + (rows,) * 2,
        out_specs=(fs_tp,) * 6 + (cols,) * 7 + (rows,) * 2,
        check_vma=False,
    )
```
